256 devices in a mesh: ep: 64 (over z, x, core), tp: 4 (over y).
Axes of the slice: x: 4, y: 4, z: 8, core: 2. Of those that a mesh axis runs over, the one named last changes fastest.
Arguments:
- queries: bfloat16 [16384, 1024], P('ep', 'tp'), may hold values from -5 to 5
- keys: bfloat16 [16384, 1024], P('ep', 'tp'), may hold values from -5 to 5
- values: bfloat16 [16384, 1024], P('ep', 'tp'), may hold values from -6 to 6
- gate_totals: float32 [16384, 8], P('ep', 'tp'), as said below
- out_proj: bfloat16 [1024, 2048], P('tp'), may hold values from -0.75 to 0.75
- moe_input: bfloat16 [24576, 2048], P('ep'), may hold values from -600 to 600
- norm_gain: float32 [2048], replicated, may hold values from 0.1 to 1.9
- routes: int32 [24576, 2], P('ep'), may hold values from 0 to 63, all different within a row; in each aligned block of 384 rows (0 to 383, 384 to 767, ...) at most 16 rows name the same one
- route_logits: float32 [24576, 2], P('ep'), may hold values from -6 to 6
- expert_gate: bfloat16 [64, 2048, 3072], P('ep', None, 'tp'), may hold values from -0.125 to 0.125
- expert_up: bfloat16 [64, 2048, 3072], P('ep', None, 'tp'), may hold values from -0.125 to 0.125
- expert_down: bfloat16 [64, 3072, 2048], P('ep', 'tp'), may hold values from -0.109375 to 0.109375
Outputs:
- mixed: bfloat16 [16384, 2048], P('ep', 'tp')
- routed: bfloat16 [24576, 2048], P('ep', 'tp')
The draws below stay inside these ranges and needn't reach their ends.
Inputs may be any that keep to these rules, and one draw needn't show every extreme that they name: `gate_totals`: along the positions, each head's values never increase. `routes`: A token names 2 different experts. Among the 384 tokens of one index of ep no expert is named more than 16 times, and in some of these blocks one expert is named exactly 16 times.
All inputs are finite; a program needn't handle non-finite values.
Results may differ from the reference program's by a relative error of at most 0.01.
Values may be sent and summed in bfloat16 or wider, within the bound.
No kernel may reach another device: no remote copies, remote signals or barrier semaphores. Data moves between devices by JAX's collectives and lax.ppermute only.
A program may use at most 128 MiB of HBM per device.

```python
import math
import jax
import jax.numpy as jnp
import numpy as np
from jax import lax

D = 2048
HEADS = 8
HD = 128
FFE = 3072
TOPK = 2
TA = 256
TB = 384
SEQUENCE_TOKENS = 16384
TOKB = 24576
EXPERTS = 64
CAP = 16
N_EP = 64
N_TP = 4


def plant_pair(key):
    base = jax.random.fold_in(key, 7)
    key_query, key_key = jax.random.split(base, 2)
    width = HEADS * HD
    queries = jnp.clip(1.7 * jax.random.normal(key_query, (SEQUENCE_TOKENS, width), jnp.float32), -5.0, 5.0)
    keys = jnp.clip(jax.random.normal(key_key, (SEQUENCE_TOKENS, width), jnp.float32), -5.0, 5.0)
    return (queries, keys)


def draw_queries(key, part):
    return plant_pair(key)[0].astype(jnp.bfloat16)


def draw_keys(key, part):
    return plant_pair(key)[1].astype(jnp.bfloat16)


def draw_gate_totals(key, part):
    key_portions = jax.random.split(jax.random.fold_in(key, 13), 7)
    order = jax.random.permutation(key_portions[0], HEADS)
    fast = (order < HEADS // 2).astype(jnp.float32)
    slow_total = jax.random.uniform(key_portions[1], (HEADS,), jnp.float32, 0.15, 0.5)
    reach = jnp.exp(jax.random.uniform(key_portions[2], (HEADS,), jnp.float32, math.log(30.0), math.log(100.0)))
    rate = fast / reach + (1.0 - fast) * slow_total / SEQUENCE_TOKENS
    device_factor = jnp.exp(jax.random.uniform(key_portions[3], (SEQUENCE_TOKENS // TA, HEADS), jnp.float32, -0.7, 0.7))
    rough = jax.random.uniform(key_portions[4], (SEQUENCE_TOKENS, HEADS), jnp.float32, 0.4, 1.6)
    log_steps = -rate[None, :] * jnp.repeat(device_factor, TA, axis=0) * rough
    arrival_rows = jax.random.randint(key_portions[5], (2,), 0, SEQUENCE_TOKENS)
    depth = jax.random.uniform(key_portions[6], (2, HEADS), jnp.float32, 0.22, 0.69)
    expert_matches = (jnp.arange(SEQUENCE_TOKENS)[:, None] == arrival_rows[None, :]).astype(jnp.float32)
    log_steps = log_steps - jnp.dot(expert_matches, depth) * (1.0 - fast)[None, :]
    return jnp.cumsum(log_steps, axis=0)


def draw_moe_input(key, part):
    key_main = jax.random.fold_in(jax.random.fold_in(key, 17), 0)
    result = jnp.clip(jax.random.normal(key_main, (TOKB, D), jnp.float32), -6.0, 6.0)
    return result.astype(jnp.bfloat16)


def block_levels(own_key, extent, shards, low, high):
    def one(position, blocks):
        steps = jax.random.uniform(jax.random.fold_in(jax.random.fold_in(own_key, 6), position), (blocks,), jnp.float32, low / len(shards), high / len(shards))
        return jnp.repeat(jnp.exp(steps), extent[position] // blocks).reshape((-1,) + (1,) * (len(extent) - position - 1))

    gain = one(*shards[0])
    for cut in shards[1:]:
        gain = gain * one(*cut)
    return gain


def deal_out(key, own, number, rows, number_of, top, most, slope):
    order = jax.random.permutation(key, number_of)
    packed, ordinary = load_shares(number_of, rows * top, most, slope, True), load_shares(number_of, rows * top, most, slope, False)
    places = jnp.arange(number_of)

    def named(tallies, turn):
        used = int((tallies > 0).sum())
        fixed = max(1, used // 4)
        moved = fixed + (places - fixed + turn * (used - fixed)) % max(1, number_of - fixed)
        return jnp.zeros((number_of,), jnp.int32).at[order[jnp.where(places < fixed, places, moved)]].set(jnp.asarray(tallies, jnp.int32))

    tallies = jnp.where(number % 4 == 0, named(packed, number // 4), named(ordinary, number - number // 4 - 1))
    mixed = jax.random.permutation(jax.random.fold_in(own, 3), number_of)
    source_of, sink = mixed[0:number_of // 2 * 2:2], mixed[1:number_of // 2 * 2:2]
    room = jnp.minimum(tallies[source_of] - 1, most - tallies[sink]) // 2
    room = jnp.where((source_of == order[0]) | (sink == order[0]) | (tallies[sink] == 0), 0, jnp.maximum(room, 0))
    moved = jax.random.randint(jax.random.fold_in(own, 4), (number_of // 2,), 0, 1 << 20) % (room + 1)
    tallies = tallies.at[source_of].add(-moved).at[sink].add(moved)
    labels = jnp.searchsorted(jnp.cumsum(tallies), jnp.arange(rows * top), side="right").astype(jnp.int32)
    listing = labels.reshape(top, rows).T
    listing = listing[jax.random.permutation(jax.random.fold_in(own, 1), rows)]
    turn = jax.random.randint(jax.random.fold_in(own, 2), (rows, 1), 0, top)
    return jnp.take_along_axis(listing, (jnp.arange(top)[None, :] + turn) % top, axis=1)


def load_shares(amount, total, limit, skew, full):
    portions = [(1 << 20) // math.isqrt(rank ** skew) + 1 for rank in range(1, amount + 1)]
    largest = limit if full else min(limit, max(-(-total // amount), total * portions[0] // sum(portions)))
    least = 1 if total - largest >= amount - 1 else 0
    counts, surplus = [largest] + [least] * (amount - 1), total - largest - least * (amount - 1)
    while surplus > 0:
        movable = [i for i in range(1, amount) if counts[i] < largest] or [i for i in range(1, amount) if counts[i] < limit]
        whole, budget = sum([portions[i] for i in movable]), surplus
        for i in movable:
            more = min(limit - counts[i], max(1, budget * portions[i] // whole), surplus)
            counts[i] = counts[i] + more
            surplus = surplus - more
    return np.array(counts)


def centred(key, shape, scale, limit, cuts=(), kind=jnp.bfloat16):
    gain = block_levels(key, shape, cuts, -0.22, 0.18) if cuts else 1.0
    values = jax.random.normal(key, shape, jnp.float32) * scale * gain
    return jnp.minimum(jnp.maximum(values, -limit), limit).astype(kind)


def setup_inputs(seed: int = 0) -> dict:
    key_of = jax.random.split(jax.random.key(seed), 13)
    queries = draw_queries(jax.random.fold_in(key_of[12], 71), 0)
    keys = draw_keys(jax.random.fold_in(key_of[12], 71), 0)
    values = centred(key_of[2], (SEQUENCE_TOKENS, HEADS * HD), 1.0, 6.0, ((0, 64), (1, 4)))
    gate_totals = draw_gate_totals(jax.random.fold_in(key_of[12], 71), 0)
    out_proj = centred(key_of[4], (HEADS * HD, D), (HEADS * HD // 16) ** -0.5, 0.75, ((0, 4),))
    moe_input = draw_moe_input(jax.random.fold_in(key_of[12], 71), 0)
    norm_gain = jnp.clip(1.0 + 0.18 * jax.random.normal(key_of[6], (D,), jnp.float32), 0.1, 1.9)
    routes_keys = jax.random.split(jax.random.fold_in(key_of[7], 1), TOKB // TB)
    routes_turns = jax.random.permutation(jax.random.fold_in(key_of[7], 3), TOKB // TB)
    routes = jax.vmap(lambda own, number: deal_out(jax.random.fold_in(key_of[7], 2), own, number, TB, EXPERTS, TOPK, CAP, 1))(routes_keys, routes_turns).reshape((TOKB, TOPK))
    route_logits = centred(key_of[8], (TOKB, TOPK), 1.5, 6.0, ((0, 64),), jnp.float32)
    expert_gate = centred(key_of[9], (EXPERTS, D, FFE), D ** -0.5, 0.125, ((0, 64), (2, 4)))
    expert_up = centred(key_of[10], (EXPERTS, D, FFE), D ** -0.5, 0.125, ((0, 64), (2, 4)))
    expert_down = centred(key_of[11], (EXPERTS, FFE, D), FFE ** -0.5, 0.109375, ((0, 64), (1, 4)))
    return {"queries": queries, "keys": keys, "values": values, "gate_totals": gate_totals, "out_proj": out_proj, "moe_input": moe_input, "norm_gain": norm_gain, "routes": routes, "route_logits": route_logits, "expert_gate": expert_gate, "expert_up": expert_up, "expert_down": expert_down}


epsilon = 1e-06

def attention_per_head(head_queries, head_keys, value_per_head, head_totals):
    block = math.gcd(SEQUENCE_TOKENS, 512)
    scale = 1.0 / math.sqrt(HD)
    key_pos = jnp.arange(SEQUENCE_TOKENS, dtype=jnp.int32)

    def one_block(index):
        start = (index * block).astype(jnp.int32)
        query_block = lax.dynamic_slice_in_dim(head_queries, start, block, 0)
        total_block = lax.dynamic_slice_in_dim(head_totals, start, block, 0)
        scores = jnp.dot(query_block, head_keys.T, preferred_element_type=jnp.float32) * scale
        scores = scores + total_block[:, None] - head_totals[None, :]
        query_pos = start + jnp.arange(block, dtype=jnp.int32)
        scores = jnp.where(key_pos[None, :] <= query_pos[:, None], scores, -jnp.inf)
        weights = jnp.exp(scores - lax.optimization_barrier(jnp.max(scores, axis=1, keepdims=True)))
        denominator = lax.optimization_barrier(jnp.sum(weights, axis=1, keepdims=True))
        summed = jnp.dot(weights.astype(jnp.bfloat16), value_per_head, preferred_element_type=jnp.float32)
        return (summed / denominator).astype(jnp.bfloat16)
    return lax.map(one_block, jnp.arange(SEQUENCE_TOKENS // block, dtype=jnp.int32)).reshape(SEQUENCE_TOKENS, HD)

def split_heads(array):
    return jnp.transpose(array.reshape(SEQUENCE_TOKENS, HEADS, HD), (1, 0, 2))

def reference(queries, keys, values, gate_totals, out_proj, moe_input, norm_gain, routes, route_logits, expert_gate, expert_up, expert_down):

    def one_head(parts):
        return attention_per_head(parts[0], parts[1], parts[2], parts[3])
    head_mix = lax.map(one_head, (split_heads(queries), split_heads(keys), split_heads(values), jnp.transpose(gate_totals)))
    group = HEADS // N_TP
    head_weights = out_proj.reshape(HEADS, HD, D)
    mixed_total = jnp.zeros((SEQUENCE_TOKENS, D), jnp.float32)
    for index in range(N_TP):
        part = jnp.einsum('hqd,hdn->qn', head_mix[index * group:(index + 1) * group].astype(jnp.float32), head_weights[index * group:(index + 1) * group].astype(jnp.float32))
        mixed_total = mixed_total + lax.optimization_barrier(part.astype(jnp.bfloat16)).astype(jnp.float32)
    mixed = mixed_total.astype(jnp.bfloat16)
    moe_float = moe_input.astype(jnp.float32)
    normed = (moe_float * lax.rsqrt(lax.optimization_barrier(jnp.mean(moe_float * moe_float, axis=1, keepdims=True)) + epsilon) * norm_gain).astype(jnp.bfloat16)
    flat_routes = routes.reshape(N_EP, TB * TOPK)
    indicator_matrix = (flat_routes[:, :, None] == jnp.arange(EXPERTS, dtype=jnp.int32)[None, None, :]).astype(jnp.int32)
    rank = lax.optimization_barrier(jnp.sum((jnp.cumsum(indicator_matrix, axis=1) - indicator_matrix) * indicator_matrix, axis=2))
    source_dev = jnp.arange(N_EP, dtype=jnp.int32)[:, None]
    slot_of = (flat_routes * (N_EP * CAP) + source_dev * CAP + rank).reshape(-1).astype(jnp.int32)
    token_of = (source_dev * TB + jnp.arange(TB * TOPK, dtype=jnp.int32)[None, :] // TOPK).reshape(-1).astype(jnp.int32)
    source = jnp.full((EXPERTS * N_EP * CAP,), TOKB, jnp.int32).at[slot_of].set(token_of)
    padded = jnp.concatenate([normed, jnp.zeros((1, D), jnp.bfloat16)], axis=0)
    quarter = FFE // N_TP

    def one_expert(expert):
        chosen = lax.dynamic_slice_in_dim(source, (expert * (N_EP * CAP)).astype(jnp.int32), N_EP * CAP, 0)
        rows = jnp.take(padded, chosen, axis=0)
        gate_rows = jnp.dot(rows, expert_gate[expert], preferred_element_type=jnp.float32)
        up_rows = jnp.dot(rows, expert_up[expert], preferred_element_type=jnp.float32)
        hidden = (jax.nn.silu(gate_rows) * up_rows).astype(jnp.bfloat16)
        down = expert_down[expert]
        total = jnp.zeros((N_EP * CAP, D), jnp.float32)
        for index in range(N_TP):
            part = jnp.dot(hidden[:, index * quarter:(index + 1) * quarter], down[index * quarter:(index + 1) * quarter], preferred_element_type=jnp.float32)
            total = total + lax.optimization_barrier(part.astype(jnp.bfloat16)).astype(jnp.float32)
        return total.astype(jnp.bfloat16)
    expert_rows = lax.map(one_expert, jnp.arange(EXPERTS, dtype=jnp.int32))
    picked = jnp.take(expert_rows.reshape(EXPERTS * N_EP * CAP, D), slot_of, axis=0).reshape(TOKB, TOPK, D)
    route_weights = jax.nn.sigmoid(route_logits - route_logits[:, ::-1])
    routed = lax.optimization_barrier(jnp.sum(picked.astype(jnp.float32) * route_weights[:, :, None], axis=1)).astype(jnp.bfloat16)
    return (mixed, routed)
```

```python
import math

import jax
import jax.numpy as jnp
from jax import lax
from jax.experimental import pallas as pl
from jax.experimental.pallas import tpu as pltpu
from jax.sharding import Mesh, PartitionSpec as P


epsilon = 1e-06
far_below = -1e30
log2e = 1.0 / math.log(2.0)
f32, bf16, i32 = jnp.float32, jnp.bfloat16, jnp.int32

NZ, NX, NC, NT = 8, 4, 2, 4
EP = ("z", "x", "c")
PLANE = ("x", "c")
EXPERTS, CAP, CH = 64, 16, 2
SLOTS = CAP // CH
ROWS = EXPERTS * SLOTS
TA, TB, D, HD = 256, 384, 2048, 128
DQ = D // NT
EXTRA = 16


def shift(value, axis, size, by):
    return lax.ppermute(value, axis, [(i, (i + by) % size) for i in range(size)])


def split3(value):
    hi = value.astype(bf16)
    rest = value - hi.astype(f32)
    mid = rest.astype(bf16)
    lo = (rest - mid.astype(f32)).astype(bf16)
    return [hi.astype(f32), mid.astype(f32), lo.astype(f32)]


def packed_rows(first, second):
    row = lax.broadcasted_iota(i32, (EXTRA, first.shape[1]), 0)
    out = jnp.zeros((EXTRA, first.shape[1]), f32)
    for n, part in enumerate(split3(first) + split3(second)):
        out = jnp.where(row == n, part, out)
    return out.astype(bf16)


def call(kernel, *, out_shape, flops=1_000_000, bytes_accessed=1_000_000, exps=0, **kw):
    return pl.pallas_call(
        kernel,
        out_shape=out_shape,
        cost_estimate=pl.CostEstimate(
            flops=flops, bytes_accessed=bytes_accessed, transcendentals=exps
        ),
        **kw,
    )


def smem():
    return pl.BlockSpec(memory_space=pltpu.SMEM)


def whole():
    return pl.BlockSpec(memory_space=pltpu.VMEM)


def pick_kernel(q_ref, x_ref, gain_ref, routes_ref, routes_t_ref, out0, out1, slots_ref):
    q = q_ref[0]
    x = x_ref[...].astype(f32)
    mean = jnp.mean(x * x, axis=1, keepdims=True)
    at = pl.multiple_of(q * DQ, DQ)
    own = x_ref[:, pl.ds(at, DQ)].astype(f32)
    normed = (own * lax.rsqrt(mean + epsilon) * gain_ref[:, pl.ds(at, DQ)]).astype(bf16)
    expert = lax.broadcasted_iota(i32, (EXPERTS, TB), 0)
    named = (routes_t_ref[0:1, :] == expert) | (routes_t_ref[1:2, :] == expert)
    row = lax.broadcasted_iota(i32, (TB, TB), 0)
    col = lax.broadcasted_iota(i32, (TB, TB), 1)
    before = (row < col).astype(f32).astype(bf16)
    earlier = jnp.dot(named.astype(f32).astype(bf16), before, preferred_element_type=f32)
    place = jnp.where(named, earlier + 1.0, 0.0).astype(bf16)
    r_row = lax.broadcasted_iota(i32, (ROWS, EXPERTS), 0)
    r_col = lax.broadcasted_iota(i32, (ROWS, EXPERTS), 1)
    spread = ((r_row // SLOTS) == r_col).astype(f32).astype(bf16)
    places = jnp.dot(spread, place, preferred_element_type=f32)
    slot = (lax.broadcasted_iota(i32, (ROWS, TB), 0) % SLOTS + 1).astype(f32)
    for n, out in enumerate((out0, out1)):
        chosen = (places == slot + float(n * SLOTS)).astype(f32).astype(bf16)
        out[...] = jnp.dot(chosen, normed, preferred_element_type=f32).astype(bf16)
    expert = lax.broadcasted_iota(i32, (TB, EXPERTS), 1)
    first, second = routes_ref[:, 0:1] == expert, routes_ref[:, 1:2] == expert
    after = (col < row).astype(f32).astype(bf16)
    earlier = jnp.dot(after, (first | second).astype(f32).astype(bf16), preferred_element_type=f32)
    for k, mine in enumerate((first, second)):
        rank = jnp.sum(jnp.where(mine, earlier, 0.0), axis=1, keepdims=True).astype(i32)
        chunk = rank // SLOTS
        slots_ref[:, k : k + 1] = (
            chunk * ROWS + routes_ref[:, k : k + 1] * SLOTS + (rank - chunk * SLOTS)
        )


def pick(q, moe_input, gain, routes):
    return call(
        pick_kernel,
        name="pick",
        in_specs=[smem(), whole(), whole(), whole(), whole()],
        out_specs=[whole()] * 3,
        out_shape=[jax.ShapeDtypeStruct((ROWS, DQ), bf16)] * CH
        + [jax.ShapeDtypeStruct((TB, 2), i32)],
        flops=2 * CH * ROWS * TB * DQ,
    )(q, moe_input, gain.reshape(1, D), routes, jnp.transpose(routes))


def expert_kernel(q_ref, own, left, right, opp_a, opp_b, wg, wu, wd, o_opp, o_right, o_left, o_own, x_s, h_s):
    step = pl.program_id(0)
    q = q_ref[0]
    half = ROWS // 2

    @pl.when(step == 0)
    def _():
        def put(rel, rows, ref):
            at = pl.multiple_of(((q + rel) % NT) * DQ, DQ)
            x_s[rows, pl.ds(at, DQ)] = ref[...]

        put(0, slice(0, ROWS), own)
        put(3, slice(0, ROWS), left)
        put(1, slice(0, ROWS), right)
        put(2, slice(0, half), opp_a)
        put(2, slice(half, ROWS), opp_b)

    for n in range(3):

        @pl.when(step == n)
        def _(n=n):
            gate = jnp.dot(x_s[...], wg[...], preferred_element_type=f32)
            up = jnp.dot(x_s[...], wu[...], preferred_element_type=f32)
            h_s[:, n * 256 : (n + 1) * 256] = (gate / (1.0 + jnp.exp(-gate)) * up).astype(bf16)

    for n, out in enumerate((o_opp, o_right, o_left, o_own)):

        @pl.when(step == 3 + n)
        def _(out=out):
            out[...] = jnp.dot(h_s[...], wd[...], preferred_element_type=f32).astype(bf16)


def out_rel(n):
    return jnp.where(n == 0, 2, jnp.where(n == 1, 1, jnp.where(n == 2, 3, 0)))


def expert(q, own, left, right, opp_a, opp_b, wg, wu, wd):
    units = wg.shape[1]
    col = lambda s, q: (0, jnp.minimum(s, 2))
    full = lambda shape: pl.BlockSpec(shape, lambda s, q: (0, 0))
    return call(
        expert_kernel,
        name="expert",
        grid_spec=pltpu.PrefetchScalarGridSpec(
            num_scalar_prefetch=1,
            grid=(7,),
            in_specs=[
                full((ROWS, DQ)),
                full((ROWS, DQ)),
                full((ROWS, DQ)),
                full((ROWS // 2, DQ)),
                full((ROWS // 2, DQ)),
                pl.BlockSpec((D, 256), col),
                pl.BlockSpec((D, 256), col),
                pl.BlockSpec(
                    (units, DQ), lambda s, q: (0, (q[0] + out_rel(jnp.maximum(s - 3, 0))) % NT)
                ),
            ],
            out_specs=[full((ROWS, DQ))] * 4,
            scratch_shapes=[pltpu.VMEM((ROWS, D), bf16), pltpu.VMEM((ROWS, units), bf16)],
        ),
        out_shape=[jax.ShapeDtypeStruct((ROWS, DQ), bf16)] * 4,
        flops=6 * ROWS * D * units,
        bytes_accessed=6 * D * units + 16 * ROWS * DQ,
        exps=ROWS * units,
    )(q, own, left, right, opp_a, opp_b, wg, wu, wd)


def combine_kernel(ret0, ret1, slots_ref, logits_ref, out_ref):
    lane = lax.broadcasted_iota(i32, (TB, CH * ROWS), 1)
    total = jnp.zeros((TB, DQ), f32)
    for k in range(2):
        chosen = (slots_ref[:, k : k + 1] == lane).astype(f32).astype(bf16)
        rows = jnp.dot(chosen[:, :ROWS], ret0[...], preferred_element_type=f32)
        rows = rows + jnp.dot(chosen[:, ROWS:], ret1[...], preferred_element_type=f32)
        other = logits_ref[:, 1 - k : 2 - k] - logits_ref[:, k : k + 1]
        total = total + rows / (1.0 + jnp.exp(other))
    out_ref[...] = total.astype(bf16)


def combine(ret0, ret1, slots, logits):
    return call(
        combine_kernel,
        name="combine",
        in_specs=[whole()] * 4,
        out_specs=whole(),
        out_shape=jax.ShapeDtypeStruct((TB, DQ), bf16),
        flops=4 * TB * CH * ROWS * DQ,
    )(ret0, ret1, slots, logits)


def pack_kernel(k_ref, v_ref, g_ref, out):
    out[0:TA, 0:256] = k_ref[...]
    out[0:TA, 256:512] = jnp.transpose(v_ref[...].astype(f32)).astype(bf16)
    gates = g_ref[...] * log2e
    out[TA : TA + EXTRA, 0:256] = packed_rows(gates[0:1, :], gates[1:2, :])
    out[TA : TA + EXTRA, 256:512] = jnp.zeros((EXTRA, 256), bf16)


def pack(keys, values, gate_totals):
    return call(
        pack_kernel,
        name="pack",
        in_specs=[whole()] * 3,
        out_specs=whole(),
        out_shape=jax.ShapeDtypeStruct((TA + EXTRA, 512), bf16),
    )(keys, values, jnp.transpose(gate_totals))


def flash_kernel(pos, q_near, q_far, *refs):
    kv_in, (out, kv_s, g_s) = refs[:9], refs[9:]
    z, x, c = pos[0], pos[1], pos[2]
    w = 2 * x + c
    for off, ref in zip((0, -1, -2, -3, 1, 2, 3), kv_in[:7]):
        kv_s[(z + off + NZ) % NZ] = ref[...]
    half = (TA + EXTRA) // 2
    kv_s[(z + 4) % NZ, 0:half, :] = kv_in[7][...]
    kv_s[(z + 4) % NZ, half : TA + EXTRA, :] = kv_in[8][...]
    for j in range(NZ):
        cols = jnp.transpose(kv_s[j, TA : TA + EXTRA, 0:256].astype(f32))
        for h in range(2):
            g = cols[:, 3 * h : 3 * h + 1] + cols[:, 3 * h + 1 : 3 * h + 2]
            g = g + cols[:, 3 * h + 2 : 3 * h + 3]
            g_s[j, :, h * HD : (h + 1) * HD] = jnp.broadcast_to(g, (TA, HD))
    scale = log2e / math.sqrt(HD)
    krow = lax.broadcasted_iota(i32, (TA, TA), 0)
    qcol = lax.broadcasted_iota(i32, (TA, TA), 1)

    def block(j, carry, queries, masked):
        new = []
        for h in range(2):
            m, l, acc = carry[h]
            cols = slice(h * HD, (h + 1) * HD)
            s = lax.dot_general(
                kv_s[j, 0:TA, cols],
                queries[h],
                (((1,), (1,)), ((), ())),
                preferred_element_type=f32,
            )
            g = g_s[j, :, cols]
            s = s * scale - jnp.concatenate([g, g], axis=1)
            if masked:
                s = jnp.where(krow <= qcol, s, far_below)
            top = jnp.maximum(m, jnp.max(s, axis=0, keepdims=True))
            p = jnp.exp2(s - top)
            keep = jnp.exp2(m - top)
            l = l * keep + jnp.sum(p, axis=0, keepdims=True)
            vt = kv_s[j, h * HD : (h + 1) * HD, 256:512]
            acc = acc * keep + jnp.dot(vt, p.astype(bf16), preferred_element_type=f32)
            new.append((m * 0.0 + top, l, acc))
        return tuple(new)

    def one(n, _):
        near = n < NX
        b = n % NX
        off = jnp.where(b == 0, 0, jnp.where(b == 1, 3, jnp.where(b == 2, 1, 2)))
        dest = 2 * ((x + off) % NX) + jnp.where(near, c, 1 - c)

        @pl.when(near)
        def _():
            run(q_near, b, dest)

        @pl.when(jnp.logical_not(near))
        def _():
            run(q_far, b, dest)

        return 0

    def run(q_ref, b, dest):
        queries = [q_ref[b, :, h * HD : (h + 1) * HD] for h in range(2)]
        start = tuple(
            (jnp.full((1, TA), far_below, f32), jnp.zeros((1, TA), f32), jnp.zeros((HD, TA), f32))
            for _ in range(2)
        )
        carry = lax.cond(dest == w, lambda: block(z, start, queries, True), lambda: start)
        count = z + (dest > w).astype(i32)
        carry = lax.fori_loop(0, count, lambda j, cy: block(j, cy, queries, False), carry)
        level = []
        for h in range(2):
            m, l, acc = carry[h]
            some = l > 0.0
            safe = jnp.where(some, l, 1.0)
            out[dest, h * HD : (h + 1) * HD, :] = (acc / safe).astype(bf16)
            level.append(jnp.where(some, m + jnp.log2(safe), far_below))
        out[dest, TA : TA + EXTRA, :] = packed_rows(level[0], level[1])

    lax.fori_loop(0, 2 * NX, one, 0)


def flash(pos, q_near, q_far, blocks):
    return call(
        flash_kernel,
        name="flash",
        in_specs=[smem()] + [whole()] * 11,
        out_specs=whole(),
        out_shape=jax.ShapeDtypeStruct((NX * NC, TA + EXTRA, 256), bf16),
        scratch_shapes=[
            pltpu.VMEM((NZ, TA + EXTRA, 512), bf16),
            pltpu.VMEM((NZ, TA, 256), f32),
        ],
        flops=20_000_000_000,
        exps=2 * NZ * NX * NC * TA * TA,
    )(pos, q_near, q_far, *blocks)


def merge_kernel(q_ref, parts, w_ref, o_opp, o_right, o_left, o_own):
    q = q_ref[0]
    n = NX * NC
    heads = []
    for h in range(2):
        level = []
        for i in range(n):
            r = parts[i, TA : TA + EXTRA, :].astype(f32)
            level.append(r[3 * h : 3 * h + 1] + r[3 * h + 1 : 3 * h + 2] + r[3 * h + 2 : 3 * h + 3])
        top = level[0]
        for v in level[1:]:
            top = jnp.maximum(top, v)
        weight = [jnp.exp2(v - top) for v in level]
        total = weight[0]
        for v in weight[1:]:
            total = total + v
        acc = jnp.zeros((HD, TA), f32)
        for i in range(n):
            acc = acc + parts[i, h * HD : (h + 1) * HD, :].astype(f32) * weight[i]
        heads.append(acc / total)
    mix = jnp.transpose(jnp.concatenate(heads, axis=0)).astype(bf16)
    for rel, out in ((2, o_opp), (1, o_right), (3, o_left), (0, o_own)):
        at = pl.multiple_of(((q + rel) % NT) * DQ, DQ)
        out[...] = jnp.dot(mix, w_ref[:, pl.ds(at, DQ)], preferred_element_type=f32).astype(bf16)


def merge(q, parts, out_proj):
    return call(
        merge_kernel,
        name="merge",
        in_specs=[smem(), whole(), whole()],
        out_specs=[whole()] * 4,
        out_shape=[jax.ShapeDtypeStruct((TA, DQ), bf16)] * 4,
        flops=2 * TA * 256 * D,
    )(q, parts, out_proj)


def gathered(own):
    half = own.shape[0] // 2
    left = shift(own, "tp", NT, 1)
    right = shift(own, "tp", NT, -1)
    opp_a = shift(left[:half], "tp", NT, 1)
    opp_b = shift(right[half:], "tp", NT, -1)
    return own, left, right, opp_a, opp_b


def summed(opp, right, left, own):
    half = opp.shape[0] // 2
    from_left = shift(opp[:half], "tp", NT, 1)
    from_right = shift(opp[half:], "tp", NT, -1)

    def plus(a, b):
        return (a.astype(f32) + b.astype(f32)).astype(bf16)

    right = jnp.concatenate([plus(right[:half], from_left), right[half:]], axis=0)
    left = jnp.concatenate([left[:half], plus(left[half:], from_right)], axis=0)
    a = shift(right, "tp", NT, 1)
    b = shift(left, "tp", NT, -1)
    return (own.astype(f32) + a.astype(f32) + b.astype(f32)).astype(bf16)


def across(value):
    rows = value.reshape(EXPERTS, SLOTS, DQ)
    return lax.all_to_all(rows, EP, 0, 0, tiled=True).reshape(ROWS, DQ)


def body(
    queries,
    keys,
    values,
    gate_totals,
    out_proj,
    moe_input,
    norm_gain,
    routes,
    route_logits,
    expert_gate,
    expert_up,
    expert_down,
):
    q = lax.axis_index("tp").astype(i32).reshape(1)
    pos = jnp.stack([lax.axis_index(a) for a in EP]).astype(i32)

    *chunks, slots = pick(q, moe_input, norm_gain, routes)
    arrived = [across(v) for v in chunks]

    near = [queries] + [shift(queries, "x", NX, s) for s in (1, -1, 2)]
    q_near = jnp.stack(near)
    q_far = shift(q_near, "c", NC, 1)
    own = pack(keys, values, gate_totals)
    up, down = [own], [own]
    for _ in range(3):
        up.append(shift(up[-1], "z", NZ, 1))
        down.append(shift(down[-1], "z", NZ, -1))
    half = (TA + EXTRA) // 2
    far = [shift(up[-1][:half], "z", NZ, 1), shift(down[-1][half:], "z", NZ, -1)]
    parts = flash(pos, q_near, q_far, up + down[1:] + far)
    parts = lax.all_to_all(parts, PLANE, 0, 0, tiled=True)
    mixed = summed(*merge(q, parts, out_proj))

    back = []
    for v in arrived:
        terms = expert(q, *gathered(v), expert_gate[0], expert_up[0], expert_down[0])
        back.append(across(summed(*terms)))
    routed = combine(*back, slots, route_logits)
    return (mixed, routed)


def solution(mesh):
    fine = Mesh(mesh.devices.reshape(NZ, NX, NC, NT), ("z", "x", "c", "tp"))
    return jax.shard_map(
        body,
        mesh=fine,
        in_specs=(
            P(EP, "tp"),
            P(EP, "tp"),
            P(EP, "tp"),
            P(EP, "tp"),
            P("tp", None),
            P(EP, None),
            P(),
            P(EP, None),
            P(EP, None),
            P(EP, None, "tp"),
            P(EP, None, "tp"),
            P(EP, "tp", None),
        ),
        out_specs=(P(EP, "tp"), P(EP, "tp")),
        check_vma=False,
    )
```
